256 devices in a mesh: sp: 32 (over z, y), dp: 8 (over x, core).
Axes of the slice: x: 4, y: 4, z: 8, core: 2. Of those that a mesh axis runs over, the one named last changes fastest.
Arguments:
- queries: bfloat16 [32768, 6144], P(('dp', 'sp')), may hold values from -360 to 360
- latent: bfloat16 [32768, 1024], P(('dp', 'sp')), may hold values from -6 to 6
- rope_key: bfloat16 [32768, 64], P(('dp', 'sp')), may hold values from -6 to 6
- latent_gain: float32 [1024], replicated, may hold values from 0.1 to 1.9
- kv_weight: bfloat16 [1024, 8192], P(None, 'dp'), may hold values from -0.1875 to 0.1875
- gate: bfloat16 [32768, 4096], P(('dp', 'sp')), may hold values from -6 to 6
- out_gain: float32 [4096], replicated, may hold values from 0.1 to 1.9
Outputs:
- attended: bfloat16 [32768, 4096], P(('dp', 'sp'))
The draws below stay inside these ranges and needn't reach their ends.
All inputs are finite; a program needn't handle non-finite values.
Results may differ from the reference program's by a relative error of at most 0.007.
Values may be sent and summed in bfloat16 or wider, within the bound.
A program may use at most 128 MiB of HBM per device.

```python
import jax
import jax.numpy as jnp
from jax import lax

HEADS = 32
NOPE = 128
ROPE = 64
VDIM = 128
KV_RANK = 1024
SEQ_LEN = 4096
TOKENS = 32768


def draw_queries(key, part):
    values = jax.random.normal(key, (TOKENS, HEADS * (NOPE + ROPE)), jnp.float32)
    values = jnp.clip(values, -6.0, 6.0)
    return values.astype(jnp.bfloat16)


def steps_of(stream_key, extent, shards, low, largest):
    loudness = 1.0
    for dim, blocks in shards:
        steps = jax.random.uniform(jax.random.fold_in(jax.random.fold_in(stream_key, 6), dim), (blocks,), jnp.float32, low / len(shards), largest / len(shards))
        loudness = loudness * jnp.repeat(jnp.exp(steps), extent[dim] // blocks).reshape((-1,) + (1,) * (len(extent) - 1 - dim))
    return loudness


def bell_draw(own_key, shape, spread, limit, pieces=(), held_as=jnp.bfloat16):
    loudness = steps_of(own_key, shape, pieces, -0.22, 0.18) if pieces else 1.0
    values = jax.random.normal(own_key, shape, jnp.float32) * spread * loudness
    return jnp.minimum(jnp.maximum(values, -limit), limit).astype(held_as)


def setup_inputs(seed: int = 0) -> dict:
    streams_of = jax.random.split(jax.random.key(seed), 8)
    return {
        "queries": draw_queries(jax.random.fold_in(streams_of[7], 71), 0),
        "latent": bell_draw(streams_of[1], (TOKENS, KV_RANK), 1.0, 6.0, ((0, 256),)),
        "rope_key": bell_draw(streams_of[2], (TOKENS, ROPE), 1.0, 6.0, ((0, 256),)),
        "latent_gain": jnp.clip(1.0 + 0.18 * jax.random.normal(streams_of[3], (KV_RANK,), jnp.float32), 0.1, 1.9),
        "kv_weight": bell_draw(streams_of[4], (KV_RANK, HEADS * (NOPE + VDIM)), KV_RANK ** -0.5, 0.1875, ((1, 8),)),
        "gate": bell_draw(streams_of[5], (TOKENS, HEADS * VDIM), 1.0, 6.0, ((0, 256),)),
        "out_gain": jnp.clip(1.0 + 0.18 * jax.random.normal(streams_of[6], (HEADS * VDIM,), jnp.float32), 0.1, 1.9),
    }


EPS = 1e-06
THETA = 10000.0

def rotary(values, position):
    half_width = values.shape[-1] // 2
    inverse = THETA ** (-jnp.arange(half_width, dtype=jnp.float32) / half_width)
    angles = position.astype(jnp.float32)[:, None] * inverse[None, :]
    if values.ndim == 3:
        angles = angles[:, None, :]
    cosine = jnp.cos(angles)
    sine_part = jnp.sin(angles)
    front_half = values[..., :half_width].astype(jnp.float32)
    back_half = values[..., half_width:].astype(jnp.float32)
    turned = jnp.concatenate([front_half * cosine - back_half * sine_part, back_half * cosine + front_half * sine_part], axis=-1)
    return turned.astype(jnp.bfloat16)

def attend(query_block, keys_plain, keys_rotated, values):
    scores = jnp.einsum('qhd,khd->hqk', query_block[..., :NOPE].astype(jnp.float32), keys_plain.astype(jnp.float32))
    scores = scores + jnp.einsum('qhr,kr->hqk', query_block[..., NOPE:].astype(jnp.float32), keys_rotated.astype(jnp.float32))
    scores = scores * (NOPE + ROPE) ** (-0.5)
    row_max = lax.optimization_barrier(jnp.max(scores, axis=-1, keepdims=True))
    raised = jnp.exp(scores - row_max)
    weights = (raised / lax.optimization_barrier(jnp.sum(raised, axis=-1, keepdims=True))).astype(jnp.bfloat16)
    result = jnp.einsum('hqk,khd->qhd', weights.astype(jnp.float32), values.astype(jnp.float32))
    return result.astype(jnp.bfloat16)

def reference(queries, latent, rope_key, latent_gain, kv_weight, gate, out_gain):
    rows_all = queries.shape[0]
    position = jnp.arange(rows_all, dtype=jnp.int32) % SEQ_LEN
    widened = latent.astype(jnp.float32)
    normed = (widened * lax.rsqrt(lax.optimization_barrier(jnp.mean(widened * widened, axis=-1, keepdims=True)) + EPS) * latent_gain.astype(jnp.float32)).astype(jnp.bfloat16)
    keyval = jnp.dot(normed, kv_weight, preferred_element_type=jnp.float32).astype(jnp.bfloat16)
    head_queries = queries.reshape(rows_all, HEADS, NOPE + ROPE)
    head_queries = jnp.concatenate([head_queries[..., :NOPE], rotary(head_queries[..., NOPE:], position)], axis=-1)
    keys_rotated = rotary(rope_key, position)
    seq_count = rows_all // SEQ_LEN
    block_rows = min(512, SEQ_LEN)
    block_count = SEQ_LEN // block_rows

    def one_sequence(operands):
        query_seq, kv_seq, rope_seq = operands
        keys_plain = kv_seq[..., :NOPE]
        values = kv_seq[..., NOPE:]
        blocks = query_seq.reshape(block_count, block_rows, HEADS, NOPE + ROPE)
        result = lax.map(lambda piece_rows: attend(piece_rows, keys_plain, rope_seq, values), blocks)
        return result.reshape(SEQ_LEN, HEADS * VDIM)
    heads_out = lax.map(one_sequence, (head_queries.reshape(seq_count, SEQ_LEN, HEADS, NOPE + ROPE), keyval.reshape(seq_count, SEQ_LEN, HEADS, NOPE + VDIM), keys_rotated.reshape(seq_count, SEQ_LEN, ROPE)))
    heads_out = heads_out.reshape(rows_all, HEADS * VDIM)
    gated_rows = heads_out.astype(jnp.float32) * jax.nn.silu(gate.astype(jnp.float32))
    scale_rows = lax.rsqrt(lax.optimization_barrier(jnp.mean(gated_rows * gated_rows, axis=-1, keepdims=True)) + EPS)
    return (gated_rows * scale_rows * out_gain.astype(jnp.float32)).astype(jnp.bfloat16)
```

```python
import functools

import jax
import jax.numpy as jnp
from jax import lax
from jax.experimental import pallas as pl
from jax.experimental.pallas import tpu as pltpu
from jax.sharding import PartitionSpec as P

HEADS = 32
NOPE = 128
ROPE = 64
VDIM = 128
RANK = 1024
EPS = 1e-06
THETA = 10000.0
LOG2E = 1.4426950408889634
SCALE = (NOPE + ROPE) ** (-0.5) * LOG2E
NX, NY, NZ = 4, 4, 8
WIDE = RANK + 128
NT = (((1,), (1,)), ((), ()))
BF16 = jnp.bfloat16
F32 = jnp.float32


def rotary(values, position):
    half_width = values.shape[-1] // 2
    inverse = THETA ** (-jnp.arange(half_width, dtype=F32) / half_width)
    angles = position.astype(F32)[:, None] * inverse[None, :]
    if values.ndim == 3:
        angles = angles[:, None, :]
    cosine = jnp.cos(angles)
    sine_part = jnp.sin(angles)
    front_half = values[..., :half_width].astype(F32)
    back_half = values[..., half_width:].astype(F32)
    turned = jnp.concatenate(
        [front_half * cosine - back_half * sine_part, back_half * cosine + front_half * sine_part],
        axis=-1,
    )
    return turned.astype(BF16)


def body(
    lat_in, q_in, w_in, gate, gain, out,
    lat, q, w, k_s, vt_s, m_s, l_s, acc_s, o_buf, o_ret, gated,
    y_send, y_recv, ring_send, ring_recv, pair_send, pair_recv,
    q_send, q_recv, w_send, w_recv, o_send, o_recv,
):
    sp, dp = lax.axis_index("sp"), lax.axis_index("dp")
    z, y = sp // NY, sp % NY
    x, core = dp // 2, dp % 2
    seq, role = y // 2, y % 2
    native = core == role
    zp, zm = (z + 1) % NZ, (z + NZ - 1) % NZ
    xp, xm = (x + 1) % NX, (x + NX - 1) % NX

    def dev(x_, core_, y_, z_):
        return {"sp": z_ * NY + y_, "dp": x_ * 2 + core_}

    def remote(src, dst, send, recv, to):
        return pltpu.make_async_remote_copy(
            src_ref=src, dst_ref=dst, send_sem=send, recv_sem=recv,
            device_id=to, device_id_type=pl.DeviceIdType.MESH,
        )

    partner = dev(x, 1 - core, y, z)
    up, down = dev(x, core, y, zp), dev(x, core, y, zm)

    def pair_of(core_, role_, t):
        is_native = core_ == role_
        slot = jnp.where(is_native, t // 2, t % 2)
        half = jnp.where(is_native, t % 2, t // 2)
        off = jnp.where(is_native, 2 * slot, 2 * slot + 1)
        return (2 * ((x + off) % NX) + role_) * 2 + half

    barrier = pltpu.get_barrier_semaphore()
    for yy in range(NY):
        for cc in range(2):
            @pl.when(jnp.logical_or(yy != y, cc != core))
            def _():
                pl.semaphore_signal(barrier, inc=1, device_id=dev(x, cc, yy, z), device_id_type=pl.DeviceIdType.MESH)
    for to in (up, down, dev(xp, 0, y, z), dev(xp, 1, y, z), dev(xm, 0, y, z), dev(xm, 1, y, z)):
        pl.semaphore_signal(barrier, inc=1, device_id=to, device_id_type=pl.DeviceIdType.MESH)
    pl.semaphore_wait(barrier, 13)

    dests = [(rr, kk) for rr in range(2) for kk in range(2)]

    def is_self(rr, kk):
        return jnp.logical_and(y == 2 * core + rr, kk == core)

    def lat_copy(rr, kk):
        return remote(
            lat_in.at[kk], lat.at[z, kk, y], y_send.at[rr, kk], y_recv.at[y],
            dev(x, kk, 2 * core + rr, z),
        )

    def q_copy(rr, kk, t):
        return remote(
            q_in.at[pair_of(kk, rr, t)], q.at[t, y], q_send.at[t, rr, kk], q_recv.at[t, y],
            dev(x, kk, 2 * core + rr, z),
        )

    for rr, kk in dests:
        @pl.when(is_self(rr, kk))
        def _():
            pltpu.make_async_copy(lat_in.at[kk], lat.at[z, kk, y], y_recv.at[y]).start()

        @pl.when(jnp.logical_not(is_self(rr, kk)))
        def _():
            lat_copy(rr, kk).start()

    def w_direct(half, plus):
        to = dev(xp if plus else xm, 1 - role, y, z)
        return remote(
            w_in.at[half], w.at[2 * half + plus], w_send.at[half, plus], w_recv.at[2 * half + plus], to
        )

    def w_relay(half):
        t_here = 1 if half == 0 else 2
        to = dev(xp if half == 0 else xm, role, y, z)
        return remote(
            w.at[t_here], w.at[2 + half], w_send.at[half, 0], w_recv.at[2 + half], to
        )

    @pl.when(native)
    def _():
        for half in range(2):
            pltpu.make_async_copy(w_in.at[half], w.at[half], w_recv.at[half]).start()
        for half in range(2):
            for plus in range(2):
                w_direct(half, plus).start()

    for t in range(4):
        for rr, kk in dests:
            @pl.when(is_self(rr, kk))
            def _():
                pltpu.make_async_copy(
                    q_in.at[pair_of(kk, rr, t)], q.at[t, y], q_recv.at[t, y]
                ).start()

            @pl.when(jnp.logical_not(is_self(rr, kk)))
            def _():
                q_copy(rr, kk, t).start()

    def cut(ref, direction, step):
        return ref.at[pl.ds(2 * direction, 2)] if step == 4 else ref

    def block_of(direction, step):
        return (z + NZ - step) % NZ if direction == 0 else (z + step) % NZ

    def ring(direction, step):
        block = cut(lat.at[block_of(direction, step - 1), core], direction, step)
        return remote(
            block, block, ring_send.at[direction, step - 1], ring_recv.at[direction, step - 1],
            up if direction == 0 else down,
        )

    def ring_arrival(direction, step):
        block = cut(lat.at[block_of(direction, step), core], direction, step)
        return remote(
            block, block, ring_send.at[direction, step - 1], ring_recv.at[direction, step - 1],
            up if direction == 0 else down,
        )

    def to_partner(direction, step):
        block = cut(lat.at[block_of(direction, step), core], direction, step)
        return remote(
            block, block, pair_send.at[direction, step], pair_recv.at[direction, step], partner
        )

    def from_partner(direction, step):
        block = cut(lat.at[block_of(direction, step), 1 - core], direction, step)
        return remote(
            block, block, pair_send.at[direction, step], pair_recv.at[direction, step], partner
        )

    for yy in range(NY):
        remote(lat_in.at[0], lat.at[z, core, yy], y_send.at[0, 0], y_recv.at[yy], partner).wait_recv()
    ring(0, 1).start()
    ring(1, 1).start()
    to_partner(0, 0).start()

    def advance(step):
        for direction in range(2):
            ring_arrival(direction, step).wait_recv()
            if step < 4:
                ring(direction, step + 1).start()
            to_partner(direction, step).start()
        for direction in range(2):
            from_partner(direction, step).wait_recv()

    def w_arrival(t):
        return remote(w_in.at[0], w.at[t], w_send.at[0, 0], w_recv.at[t], partner)

    m_s[...] = jnp.full_like(m_s, -jnp.inf)
    l_s[...] = jnp.zeros_like(l_s)
    acc_s[...] = jnp.zeros_like(acc_s)
    lane = lax.broadcasted_iota(jnp.int32, (1, 128), 1)

    def unit(t, za, zb):
        for i, zz in enumerate((za, zb)):
            lz = lat[zz].reshape(512, WIDE)[:, :RANK]
            keys = lax.dot_general(lz, w[t, :256], NT, preferred_element_type=F32)
            k_s[i * 512:(i + 1) * 512, :] = keys.astype(BF16)
            vals = lax.dot_general(w[t, 256:], lz, NT, preferred_element_type=F32)
            vt_s[:, i * 512:(i + 1) * 512] = vals.astype(BF16)
        turned = jnp.concatenate(
            [lat[zz].reshape(512, WIDE)[:, RANK:] for zz in (za, zb)], axis=0
        )
        for hh in range(2):
            mask = lane < 64 if hh == 0 else lane >= 64
            key = jnp.concatenate(
                [k_s[:, hh * 128:(hh + 1) * 128], jnp.where(mask, turned, jnp.zeros_like(turned))], axis=1
            )
            query = jnp.concatenate(
                [
                    jnp.concatenate([q[t, yy, hh], q[t, yy, 2]], axis=1)
                    for yy in range(NY)
                ],
                axis=0,
            )
            s = lax.dot_general(key, query, NT, preferred_element_type=F32)
            m_old = m_s[t, hh]
            m_new = jnp.maximum(m_old, jnp.max(s, axis=0, keepdims=True) * SCALE)
            p = jnp.exp2(s * SCALE - m_new)
            shrink = jnp.exp2(m_old - m_new)
            l_s[t, hh] = l_s[t, hh] * shrink + jnp.sum(p, axis=0, keepdims=True)
            m_s[t, hh] = m_new
            acc_s[t, hh] = acc_s[t, hh] * shrink + jnp.dot(
                vt_s[hh * 128:(hh + 1) * 128, :], p.astype(BF16), preferred_element_type=F32
            )

    def o_copy(t, yy):
        return remote(
            o_buf.at[t, yy], o_ret.at[pair_of(core, role, t)], o_send.at[t, yy],
            o_recv.at[pair_of(core, role, t)], dev(x, seq, yy, z),
        )

    def o_self(yy):
        return jnp.logical_and(yy == y, seq == core)

    @pl.when(jnp.logical_not(native))
    def _():
        w_arrival(1).wait_recv()
        w_relay(0).start()

    from_partner(0, 0).wait_recv()

    @pl.loop(0, 4)
    def _(step):
        for j in range(4):
            @pl.when(step == j)
            def _():
                advance(j + 1)
        za = jnp.where(step == 3, z, (z + NZ - 1 - step) % NZ)
        zb = (z + 1 + step) % NZ

        @pl.loop(0, 4)
        def _(t):
            @pl.when(step == 0)
            def _():
                @pl.when(jnp.logical_or(native, t != 1))
                def _():
                    w_arrival(t).wait_recv()

                @pl.when(jnp.logical_and(jnp.logical_not(native), t == 2))
                def _():
                    w_relay(1).start()

                for yy in range(NY):
                    remote(q_in.at[0], q.at[t, yy], q_send.at[0, 0, 0], q_recv.at[t, yy], partner).wait_recv()

            unit(t, za, zb)

            @pl.when(step == 3)
            def _():
                for hh in range(2):
                    r = acc_s[t, hh] / l_s[t, hh]
                    for yy in range(NY):
                        piece = r[:, yy * 128:(yy + 1) * 128].T.astype(BF16)
                        o_buf[t, yy, hh] = piece

                        @pl.when(o_self(yy))
                        def _():
                            o_ret[pair_of(core, role, t), hh] = piece
                for yy in range(NY):
                    @pl.when(jnp.logical_not(o_self(yy)))
                    def _():
                        o_copy(t, yy).start()

    total = jnp.zeros((128, 128), F32)
    for t in range(4):
        for rr, kk in dests:
            g = pair_of(kk, rr, t)

            @pl.when(jnp.logical_not(is_self(rr, kk)))
            def _():
                remote(
                    o_buf.at[0, 0], o_ret.at[g], o_send.at[0, 0], o_recv.at[g], partner
                ).wait_recv()
    for h in range(HEADS):
        v = gate[:, h * 128:(h + 1) * 128].astype(F32)
        piece = o_ret[h // 2, h % 2].astype(F32) * (v / (1.0 + jnp.exp(-v)))
        gated[:, h * 128:(h + 1) * 128] = piece
        total = total + piece * piece
    mean = jnp.sum(total, axis=1, keepdims=True) / (HEADS * VDIM)
    scale = lax.rsqrt(mean + EPS)
    for h in range(HEADS):
        cols = slice(h * 128, (h + 1) * 128)
        out[:, cols] = (gated[:, cols] * scale * gain[:, cols]).astype(BF16)

    for rr, kk in dests:
        @pl.when(jnp.logical_not(is_self(rr, kk)))
        def _():
            lat_copy(rr, kk).wait_send()
            for t in range(4):
                q_copy(rr, kk, t).wait_send()

    @pl.when(native)
    def _():
        for half in range(2):
            for plus in range(2):
                w_direct(half, plus).wait_send()

    @pl.when(jnp.logical_not(native))
    def _():
        w_relay(0).wait_send()
        w_relay(1).wait_send()

    to_partner(0, 0).wait_send()
    for direction in range(2):
        for step in range(1, 5):
            ring(direction, step).wait_send()
            to_partner(direction, step).wait_send()
    for t in range(4):
        for yy in range(NY):
            @pl.when(jnp.logical_not(o_self(yy)))
            def _():
                o_copy(t, yy).wait_send()


def per_device(queries, latent, rope_key, latent_gain, kv_weight, gate, out_gain):
    own = queries.shape[0]
    position = lax.axis_index("sp") * own + jnp.arange(own, dtype=jnp.int32)
    widened = latent.astype(F32)
    normed = (
        widened * lax.rsqrt(jnp.mean(widened * widened, axis=-1, keepdims=True) + EPS) * latent_gain
    ).astype(BF16)
    turned_key = rotary(rope_key, position)
    lat_in = jnp.concatenate([normed, turned_key, turned_key], axis=1).reshape(2, 64, WIDE)
    heads = queries.reshape(own, HEADS, NOPE + ROPE)
    turned = rotary(heads[..., NOPE:], position).reshape(own, HEADS // 2, 1, 128)
    plain = heads[..., :NOPE].reshape(own, HEADS // 2, 2, 128)
    q_in = jnp.concatenate([plain, turned], axis=2).transpose(1, 2, 0, 3)
    w_in = kv_weight.reshape(RANK, 2, 2, 2, 128).transpose(1, 3, 2, 4, 0).reshape(2, 512, RANK)
    any_spec = pl.BlockSpec(memory_space=pl.ANY)
    vmem_spec = pl.BlockSpec(memory_space=pltpu.VMEM)
    dma = pltpu.SemaphoreType.DMA
    return pl.pallas_call(
        body,
        out_shape=jax.ShapeDtypeStruct((own, HEADS * VDIM), BF16),
        in_specs=[any_spec, any_spec, any_spec, vmem_spec, vmem_spec],
        out_specs=vmem_spec,
        scratch_shapes=[
            pltpu.VMEM((NZ, 2, NY, 64, WIDE), BF16),
            pltpu.VMEM((4, NY, 3, 128, 128), BF16),
            pltpu.VMEM((4, 512, RANK), BF16),
            pltpu.VMEM((1024, 256), BF16),
            pltpu.VMEM((256, 1024), BF16),
            pltpu.VMEM((4, 2, 1, 512), F32),
            pltpu.VMEM((4, 2, 1, 512), F32),
            pltpu.VMEM((4, 2, 128, 512), F32),
            pltpu.VMEM((4, NY, 2, 128, 128), BF16),
            pltpu.VMEM((16, 2, 128, 128), BF16),
            pltpu.VMEM((own, HEADS * VDIM), F32),
            dma((2, 2)), dma((NY,)), dma((2, 4)), dma((2, 4)), dma((2, 5)), dma((2, 5)),
            dma((4, 2, 2)), dma((4, NY)), dma((2, 2)), dma((4,)), dma((4, NY)), dma((16,)),
        ],
        compiler_params=pltpu.CompilerParams(
            collective_id=0, has_side_effects=True, vmem_limit_bytes=60 * 2**20
        ),
        cost_estimate=pl.CostEstimate(flops=30 * 10**9, bytes_accessed=10**7, transcendentals=0),
        name="latent_attention",
    )(lat_in, q_in, w_in, gate, out_gain.reshape(1, -1))


def solution(mesh):
    return jax.shard_map(
        per_device,
        mesh=mesh,
        in_specs=(
            P(("dp", "sp"), None),
            P(("dp", "sp"), None),
            P(("dp", "sp"), None),
            P(),
            P(None, "dp"),
            P(("dp", "sp"), None),
            P(),
        ),
        out_specs=P(("dp", "sp"), None),
        check_vma=False,
    )
```

```python
import functools

import jax
import jax.numpy as jnp
from jax import lax
from jax.experimental import pallas as pl
from jax.experimental.pallas import tpu as pltpu
from jax.sharding import PartitionSpec as P

HEADS = 32
NOPE = 128
ROPE = 64
VDIM = 128
RANK = 1024
EPS = 1e-06
THETA = 10000.0
LOG2E = 1.4426950408889634
SCALE = (NOPE + ROPE) ** (-0.5) * LOG2E
NX, NY, NZ = 4, 4, 8
WIDE = RANK + 128
NT = (((1,), (1,)), ((), ()))
BF16 = jnp.bfloat16
AWAY = (0, 1, 3, 2)
STEP_OF = (0, 0, 1, 1, 0, 1, 2, 2, 0, 1, 2, 2, 3, 3, 3, 3, 4, 4, 4, 4)
PLACE_OF = (0, 1, 0, 1, 2, 2, 0, 1, 3, 3, 2, 3, 0, 1, 2, 3, 0, 1, 2, 3)
FIRST_USE = tuple(int(t not in PLACE_OF[:u]) for u, t in enumerate(PLACE_OF))
ARRIVALS = {
    0: ((1, 0), (1, 1)), 1: ((1, 2), (1, 3)),
    2: ((2, 0),), 3: ((2, 1),), 4: ((2, 2),), 5: ((2, 3),),
    7: ((3, 0),), 8: ((3, 1),), 9: ((3, 2),), 10: ((3, 3),),
    12: ((4, 0), (4, 2)), 13: ((4, 1), (4, 3)),
}
F32 = jnp.float32


def pick(table, index):
    value = jnp.int32(table[0])
    for i, entry in enumerate(table[1:], 1):
        value = jnp.where(index == i, jnp.int32(entry), value)
    return value


def rotary(values, position):
    half_width = values.shape[-1] // 2
    inverse = THETA ** (-jnp.arange(half_width, dtype=F32) / half_width)
    angles = position.astype(F32)[:, None] * inverse[None, :]
    if values.ndim == 3:
        angles = angles[:, None, :]
    cosine = jnp.cos(angles)
    sine_part = jnp.sin(angles)
    front_half = values[..., :half_width].astype(F32)
    back_half = values[..., half_width:].astype(F32)
    turned = jnp.concatenate(
        [front_half * cosine - back_half * sine_part, back_half * cosine + front_half * sine_part],
        axis=-1,
    )
    return turned.astype(BF16)


def body(
    lat_in, q_in, w_in, gate, gain, out,
    lat, q, qt, w, k_s, vt_s, s_s, p_s, m_s, l_s, acc_s, o_buf, o_ret, gated,
    y_send, y_recv, ring_send, ring_recv, pair_send, pair_recv,
    q_send, q_recv, w_send, w_recv, o_send, o_recv,
):
    sp, dp = lax.axis_index("sp"), lax.axis_index("dp")
    z, y = sp // NY, sp % NY
    x, core = dp // 2, dp % 2
    seq, role = y // 2, y % 2
    native = core == role
    zp, zm = (z + 1) % NZ, (z + NZ - 1) % NZ
    xp, xm = (x + 1) % NX, (x + NX - 1) % NX

    def dev(x_, core_, y_, z_):
        return {"sp": z_ * NY + y_, "dp": x_ * 2 + core_}

    def remote(src, dst, send, recv, to):
        return pltpu.make_async_remote_copy(
            src_ref=src, dst_ref=dst, send_sem=send, recv_sem=recv,
            device_id=to, device_id_type=pl.DeviceIdType.MESH,
        )

    partner = dev(x, 1 - core, y, z)
    up, down = dev(x, core, y, zp), dev(x, core, y, zm)

    def pair_of(core_, role_, t):
        is_native = core_ == role_
        slot = jnp.where(is_native, t // 2, t % 2)
        half = jnp.where(is_native, t % 2, t // 2)
        off = jnp.where(is_native, 2 * slot, 2 * slot + 1)
        return (2 * ((x + off) % NX) + role_) * 2 + half

    barrier = pltpu.get_barrier_semaphore()
    for yy in range(NY):
        for cc in range(2):
            @pl.when(jnp.logical_or(yy != y, cc != core))
            def _():
                pl.semaphore_signal(barrier, inc=1, device_id=dev(x, cc, yy, z), device_id_type=pl.DeviceIdType.MESH)
    for to in (up, down, dev(xp, 0, y, z), dev(xp, 1, y, z), dev(xm, 0, y, z), dev(xm, 1, y, z)):
        pl.semaphore_signal(barrier, inc=1, device_id=to, device_id_type=pl.DeviceIdType.MESH)
    pl.semaphore_wait(barrier, 13)

    dests = [(rr, kk) for rr in range(2) for kk in range(2)]

    def is_self(rr, kk):
        return jnp.logical_and(y == 2 * core + rr, kk == core)

    def lat_copy(rr, kk):
        return remote(
            lat_in.at[kk], lat.at[z, kk, y], y_send.at[rr, kk], y_recv.at[y],
            dev(x, kk, 2 * core + rr, z),
        )

    def q_copy(rr, kk, t):
        return remote(
            q_in.at[pair_of(kk, rr, t)], q.at[t, y], q_send.at[t, rr, kk], q_recv.at[t, y],
            dev(x, kk, 2 * core + rr, z),
        )

    for rr, kk in dests:
        @pl.when(is_self(rr, kk))
        def _():
            pltpu.make_async_copy(lat_in.at[kk], lat.at[z, kk, y], y_recv.at[y]).start()

        @pl.when(jnp.logical_not(is_self(rr, kk)))
        def _():
            lat_copy(rr, kk).start()

    def w_half(half):
        return w_in.at[:, pl.ds(512 * half, 512)]

    def w_direct(half, plus):
        to = dev(xp if plus else xm, 1 - role, y, z)
        return remote(
            w_half(half), w.at[2 * half + plus], w_send.at[half, plus], w_recv.at[2 * half + plus], to
        )

    def w_relay(half):
        t_here = 1 if half == 0 else 2
        to = dev(xp if half == 0 else xm, role, y, z)
        return remote(
            w.at[t_here], w.at[2 + half], w_send.at[half, 0], w_recv.at[2 + half], to
        )

    @pl.when(native)
    def _():
        for half in range(2):
            pltpu.make_async_copy(w_half(half), w.at[half], w_recv.at[half]).start()
        w_direct(0, 0).start()
        w_direct(0, 1).start()
        w_direct(1, 0).start()

    for t in range(4):
        for rr, kk in dests:
            @pl.when(is_self(rr, kk))
            def _():
                pltpu.make_async_copy(
                    q_in.at[pair_of(kk, rr, t)], q.at[t, y], q_recv.at[t, y]
                ).start()

            @pl.when(jnp.logical_not(is_self(rr, kk)))
            def _():
                q_copy(rr, kk, t).start()

    def source_y(i):
        return (y + AWAY[i]) % NY

    def block_of(direction, step):
        return (z + NZ - step) % NZ if direction == 0 else (z + step) % NZ

    def ring_copy(direction, step, i, have):
        piece = lat.at[block_of(direction, step - have), core, source_y(i)]
        at = (direction, step - 1, i)
        return remote(piece, piece, ring_send.at[at], ring_recv.at[at], up if direction == 0 else down)

    def ring(direction, step, i):
        return ring_copy(direction, step, i, 1)

    def pair_copy(direction, step, i, half):
        piece = lat.at[block_of(direction, step), half, source_y(i)]
        at = (direction, step, i)
        return remote(piece, piece, pair_send.at[at], pair_recv.at[at], partner)

    def carried(direction, step, i):
        return step < 4 or i // 2 == direction

    def arrive(direction, step, i):
        ring_copy(direction, step, i, 0).wait_recv()
        if step < 4 and carried(direction, step + 1, i):
            ring(direction, step + 1, i).start()
        pair_copy(direction, step, i, core).start()

    def from_partner(step):
        for direction in range(1 if step == 0 else 2):
            for i in range(4):
                if carried(direction, step, i):
                    pair_copy(direction, step, i, 1 - core).wait_recv()

    for i in range(4):
        remote(
            lat_in.at[0], lat.at[z, core, source_y(i)], y_send.at[0, 0], y_recv.at[source_y(i)], partner
        ).wait_recv()
        ring(0, 1, i).start()
        ring(1, 1, i).start()
        pair_copy(0, 0, i, core).start()

    def w_arrival(t):
        return remote(w.at[0], w.at[t], w_send.at[0, 0], w_recv.at[t], partner)

    m_s[...] = jnp.full_like(m_s, -jnp.inf)
    l_s[...] = jnp.zeros_like(l_s)
    acc_s[...] = jnp.zeros_like(acc_s)
    lane = lax.broadcasted_iota(jnp.int32, (1, 128), 1)

    def unit(t, blocks):
        n = 512 * len(blocks)
        wk = jnp.concatenate([w[t, :, 0:128], w[t, :, 256:384]], axis=1)
        wv = jnp.concatenate([w[t, :, 128:256], w[t, :, 384:512]], axis=1)
        chunks = range(len(blocks))
        rows = [slice(c * 512, (c + 1) * 512) for c in chunks]

        def block(c):
            return lat[blocks[c]].reshape(512, WIDE)

        def scores(hh, c):
            turned = block(c)[:, RANK:]
            mask = lane < 64 if hh == 0 else lane >= 64
            key = jnp.concatenate(
                [k_s[rows[c], hh * 128:(hh + 1) * 128], jnp.where(mask, turned, jnp.zeros_like(turned))],
                axis=1,
            )
            s = jnp.dot(key, qt[t, hh], preferred_element_type=F32)
            s_s[hh, rows[c], :] = s
            top = s[0:8]
            for g in range(1, 64):
                top = jnp.maximum(top, s[g * 8:(g + 1) * 8])
            return top

        def peak(hh, tops):
            top = functools.reduce(jnp.maximum, tops)
            m_old = m_s[t, hh]
            m_new = jnp.maximum(m_old, jnp.max(top, axis=0, keepdims=True) * SCALE)
            m_s[t, hh] = m_new
            return m_new, jnp.exp2(m_old - m_new)

        def raise_(hh, c, m_new):
            total = jnp.zeros((8, 512), F32)
            low = jnp.broadcast_to(m_new, (8, 512))
            for g in range(32):
                row = c * 512 + g * 16
                first = jnp.exp2(s_s[hh, row:row + 8, :] * SCALE - low)
                second = jnp.exp2(s_s[hh, row + 8:row + 16, :] * SCALE - low)
                total = total + (first + second)
                p_s[hh, row:row + 16, :] = jnp.concatenate([first, second], axis=0).astype(BF16)
            return total

        def values(c):
            v = jnp.dot(block(c)[:, :RANK], wv, preferred_element_type=F32).astype(BF16)
            vt_s[:, rows[c]] = v.T

        def finish(hh, sums, shrink):
            l_s[t, hh] = l_s[t, hh] * shrink + jnp.sum(
                functools.reduce(jnp.add, sums), axis=0, keepdims=True
            )
            acc_s[t, hh] = acc_s[t, hh] * shrink + jnp.dot(
                vt_s[hh * 128:(hh + 1) * 128, :n], p_s[hh, :n], preferred_element_type=F32
            )

        for c in chunks:
            k_s[rows[c], :] = jnp.dot(block(c)[:, :RANK], wk, preferred_element_type=F32).astype(BF16)
        m_a, shrink_a = peak(0, [scores(0, c) for c in chunks])
        tops, sums_a, sums_b = [], [], []
        for c in chunks:
            tops.append(scores(1, c))
            sums_a.append(raise_(0, c, m_a))
        m_b, shrink_b = peak(1, tops)
        for c in chunks:
            values(c)
            sums_b.append(raise_(1, c, m_b))
        finish(0, sums_a, shrink_a)
        finish(1, sums_b, shrink_b)

    def o_copy(t, yy):
        return remote(
            o_buf.at[t, yy], o_ret.at[pair_of(core, role, t)], o_send.at[t, yy],
            o_recv.at[pair_of(core, role, t)], dev(x, seq, yy, z),
        )

    def o_self(yy):
        return jnp.logical_and(yy == y, seq == core)

    @pl.when(jnp.logical_not(native))
    def _():
        w_arrival(1).wait_recv()
        w_relay(0).start()

    from_partner(0)

    @pl.loop(0, len(STEP_OF))
    def _(u):
        step = pick(STEP_OF, u)
        t = pick(PLACE_OF, u)

        @pl.when(pick(FIRST_USE, u) == 1)
        def _():
            @pl.when(jnp.logical_or(native, jnp.logical_or(t == 0, t == 3)))
            def _():
                w_arrival(t).wait_recv()

            for yy in range(NY):
                remote(q_in.at[0], q.at[t, yy], q_send.at[0, 0, 0], q_recv.at[t, yy], partner).wait_recv()
            for hh in range(2):
                rows = [jnp.concatenate([q[t, yy, hh], q[t, yy, 2]], axis=1) for yy in range(NY)]
                qt[t, hh] = jnp.concatenate(rows, axis=0).T

        for j, first in ((1, 2), (2, 6), (3, 12), (4, 16)):
            @pl.when(u == first)
            def _():
                from_partner(j)

        single = jnp.logical_or(step == 0, step == 4)

        @pl.when(single)
        def _():
            unit(t, [(z + step) % NZ])

        @pl.when(jnp.logical_not(single))
        def _():
            unit(t, [(z + NZ - step) % NZ, (z + step) % NZ])

        for at, what in ARRIVALS.items():
            @pl.when(u == at)
            def _():
                for j, i in what:
                    for direction in range(2):
                        if carried(direction, j, i):
                            arrive(direction, j, i)

        @pl.when(jnp.logical_and(native, u == 1))
        def _():
            w_direct(1, 1).start()

        @pl.when(jnp.logical_and(jnp.logical_not(native), u == 3))
        def _():
            w_arrival(2).wait_recv()
            w_relay(1).start()

        @pl.when(step == 4)
        def _():
            for hh in range(2):
                r = acc_s[t, hh] / l_s[t, hh]
                for yy in range(NY):
                    piece = r[:, yy * 128:(yy + 1) * 128].T.astype(BF16)
                    o_buf[t, yy, hh] = piece

                    @pl.when(o_self(yy))
                    def _():
                        o_ret[pair_of(core, role, t), hh] = piece
            for yy in range(NY):
                @pl.when(jnp.logical_not(o_self(yy)))
                def _():
                    o_copy(t, yy).start()

    total = jnp.zeros((128, 128), F32)
    for t in range(4):
        for rr, kk in dests:
            g = pair_of(kk, rr, t)

            @pl.when(jnp.logical_not(is_self(rr, kk)))
            def _():
                remote(
                    o_buf.at[0, 0], o_ret.at[g], o_send.at[0, 0], o_recv.at[g], partner
                ).wait_recv()
    for h in range(HEADS):
        v = gate[:, h * 128:(h + 1) * 128].astype(F32)
        piece = o_ret[h // 2, h % 2].astype(F32) * (v / (1.0 + jnp.exp(-v)))
        gated[:, h * 128:(h + 1) * 128] = piece
        total = total + piece * piece
    mean = jnp.sum(total, axis=1, keepdims=True) / (HEADS * VDIM)
    scale = lax.rsqrt(mean + EPS)
    for h in range(HEADS):
        cols = slice(h * 128, (h + 1) * 128)
        out[:, cols] = (gated[:, cols] * scale * gain[:, cols]).astype(BF16)

    for rr, kk in dests:
        @pl.when(jnp.logical_not(is_self(rr, kk)))
        def _():
            lat_copy(rr, kk).wait_send()
            for t in range(4):
                q_copy(rr, kk, t).wait_send()

    @pl.when(native)
    def _():
        for half in range(2):
            for plus in range(2):
                w_direct(half, plus).wait_send()

    @pl.when(jnp.logical_not(native))
    def _():
        w_relay(0).wait_send()
        w_relay(1).wait_send()

    for i in range(4):
        pair_copy(0, 0, i, core).wait_send()
        for direction in range(2):
            for step in range(1, 5):
                if carried(direction, step, i):
                    ring(direction, step, i).wait_send()
                    pair_copy(direction, step, i, core).wait_send()
    for t in range(4):
        for yy in range(NY):
            @pl.when(jnp.logical_not(o_self(yy)))
            def _():
                o_copy(t, yy).wait_send()


def per_device(queries, latent, rope_key, latent_gain, kv_weight, gate, out_gain):
    own = queries.shape[0]
    position = lax.axis_index("sp") * own + jnp.arange(own, dtype=jnp.int32)
    widened = latent.astype(F32)
    normed = (
        widened * lax.rsqrt(jnp.mean(widened * widened, axis=-1, keepdims=True) + EPS) * latent_gain
    ).astype(BF16)
    turned_key = rotary(rope_key, position)
    lat_in = jnp.concatenate([normed, turned_key, turned_key], axis=1).reshape(2, 64, WIDE)
    heads = queries.reshape(own, HEADS, NOPE + ROPE)
    turned = rotary(heads[..., NOPE:], position).reshape(own, HEADS // 2, 1, 128)
    plain = heads[..., :NOPE].reshape(own, HEADS // 2, 2, 128)
    q_in = jnp.concatenate([plain, turned], axis=2).transpose(1, 2, 0, 3)
    any_spec = pl.BlockSpec(memory_space=pl.ANY)
    vmem_spec = pl.BlockSpec(memory_space=pltpu.VMEM)
    dma = pltpu.SemaphoreType.DMA
    return pl.pallas_call(
        body,
        out_shape=jax.ShapeDtypeStruct((own, HEADS * VDIM), BF16),
        in_specs=[any_spec, any_spec, any_spec, vmem_spec, vmem_spec],
        out_specs=vmem_spec,
        scratch_shapes=[
            pltpu.VMEM((NZ, 2, NY, 64, WIDE), BF16),
            pltpu.VMEM((4, NY, 3, 128, 128), BF16),
            pltpu.VMEM((4, 2, 256, 512), BF16),
            pltpu.VMEM((4, RANK, 512), BF16),
            pltpu.VMEM((1024, 256), BF16),
            pltpu.VMEM((256, 1024), BF16),
            pltpu.VMEM((2, 1024, 512), F32),
            pltpu.VMEM((2, 1024, 512), BF16),
            pltpu.VMEM((4, 2, 1, 512), F32),
            pltpu.VMEM((4, 2, 1, 512), F32),
            pltpu.VMEM((4, 2, 128, 512), F32),
            pltpu.VMEM((4, NY, 2, 128, 128), BF16),
            pltpu.VMEM((16, 2, 128, 128), BF16),
            pltpu.VMEM((own, HEADS * VDIM), F32),
            dma((2, 2)), dma((NY,)), dma((2, 4, 4)), dma((2, 4, 4)), dma((2, 5, 4)), dma((2, 5, 4)),
            dma((4, 2, 2)), dma((4, NY)), dma((2, 2)), dma((4,)), dma((4, NY)), dma((16,)),
        ],
        compiler_params=pltpu.CompilerParams(
            collective_id=0, has_side_effects=True, vmem_limit_bytes=60 * 2**20
        ),
        cost_estimate=pl.CostEstimate(flops=30 * 10**9, bytes_accessed=10**7, transcendentals=0),
        name="latent_attention",
    )(lat_in, q_in, kv_weight, gate, out_gain.reshape(1, -1))


def solution(mesh):
    return jax.shard_map(
        per_device,
        mesh=mesh,
        in_specs=(
            P(("dp", "sp"), None),
            P(("dp", "sp"), None),
            P(("dp", "sp"), None),
            P(),
            P(None, "dp"),
            P(("dp", "sp"), None),
            P(),
        ),
        out_specs=P(("dp", "sp"), None),
        check_vma=False,
    )
```

```python
import functools

import jax
import jax.numpy as jnp
from jax import lax
from jax.experimental import pallas as pl
from jax.experimental.pallas import tpu as pltpu
from jax.sharding import PartitionSpec as P

HEADS = 32
NOPE = 128
ROPE = 64
VDIM = 128
RANK = 1024
EPS = 1e-06
THETA = 10000.0
LOG2E = 1.4426950408889634
SCALE = (NOPE + ROPE) ** (-0.5) * LOG2E
NX, NY, NZ = 4, 4, 8
WIDE = RANK + 128
NT = (((1,), (1,)), ((), ()))
BF16 = jnp.bfloat16
AWAY = (0, 1, 3, 2)
STEP_OF = (0, 0, 1, 1, 0, 1, 2, 2, 2, 0, 1, 2, 3, 3, 3, 3, 4, 4, 4, 4)
PLACE_OF = (0, 1, 0, 1, 2, 2, 0, 1, 2, 3, 3, 3, 0, 1, 2, 3, 0, 1, 2, 3)
FIRST_USE = tuple(int(t not in PLACE_OF[:u]) for u, t in enumerate(PLACE_OF))
ARRIVALS = {
    0: ((1, 0), (1, 1)), 1: ((1, 2), (1, 3)),
    2: ((2, 0),), 3: ((2, 1),), 4: ((2, 2),), 5: ((2, 3),),
    7: ((3, 0),), 8: ((3, 1),), 9: ((3, 2),), 10: ((3, 3),),
    12: ((4, 0), (4, 2)), 13: ((4, 1), (4, 3)),
}
F32 = jnp.float32


def pick(table, index):
    value = jnp.int32(table[0])
    for i, entry in enumerate(table[1:], 1):
        value = jnp.where(index == i, jnp.int32(entry), value)
    return value


def body(
    queries, latent, rope_key, latent_gain, cosine, sine, w_in, gate, gain, out,
    lat_in, q_in, lat, q, qt, w, k_s, vt_s, s_s, p_s, m_s, l_s, acc_s, o_buf, o_ret, gated,
    y_send, y_recv, ring_send, ring_recv, pair_send, pair_recv,
    q_send, q_recv, w_send, w_recv, o_send, o_recv,
):
    sp, dp = lax.axis_index("sp"), lax.axis_index("dp")
    z, y = sp // NY, sp % NY
    x, core = dp // 2, dp % 2
    seq, role = y // 2, y % 2
    native = core == role
    zp, zm = (z + 1) % NZ, (z + NZ - 1) % NZ
    xp, xm = (x + 1) % NX, (x + NX - 1) % NX

    def dev(x_, core_, y_, z_):
        return {"sp": z_ * NY + y_, "dp": x_ * 2 + core_}

    def remote(src, dst, send, recv, to):
        return pltpu.make_async_remote_copy(
            src_ref=src, dst_ref=dst, send_sem=send, recv_sem=recv,
            device_id=to, device_id_type=pl.DeviceIdType.MESH,
        )

    partner = dev(x, 1 - core, y, z)
    up, down = dev(x, core, y, zp), dev(x, core, y, zm)

    def pair_of(core_, role_, t):
        is_native = core_ == role_
        slot = jnp.where(is_native, t // 2, t % 2)
        half = jnp.where(is_native, t % 2, t // 2)
        off = jnp.where(is_native, 2 * slot, 2 * slot + 1)
        return (2 * ((x + off) % NX) + role_) * 2 + half

    barrier = pltpu.get_barrier_semaphore()
    for yy in range(NY):
        for cc in range(2):
            @pl.when(jnp.logical_or(yy != y, cc != core))
            def _():
                pl.semaphore_signal(barrier, inc=1, device_id=dev(x, cc, yy, z), device_id_type=pl.DeviceIdType.MESH)
    for to in (up, down, dev(xp, 0, y, z), dev(xp, 1, y, z), dev(xm, 0, y, z), dev(xm, 1, y, z)):
        pl.semaphore_signal(barrier, inc=1, device_id=to, device_id_type=pl.DeviceIdType.MESH)

    @pl.when(native)
    def _():
        for half in range(2):
            pltpu.make_async_copy(w_in.at[:, pl.ds(512 * half, 512)], w.at[half], w_recv.at[half]).start()

    lane = lax.broadcasted_iota(jnp.int32, (1, 128), 1)

    def rotated(pair):
        other = jnp.where(lane % 64 < 32, pltpu.roll(pair, 96, 1), pltpu.roll(pair, 32, 1))
        return (pair * cosine[...] + other * sine[...]).astype(BF16)

    wide = latent[...].astype(F32)
    level = lax.rsqrt(jnp.mean(wide * wide, axis=1, keepdims=True) + EPS)
    normed = (wide * level * latent_gain[...]).astype(BF16)
    key = rope_key[...].astype(F32)
    turned_key = rotated(jnp.concatenate([key, key], axis=1))
    for half in range(2):
        rows = slice(half * 64, (half + 1) * 64)
        lat_in[half, :, :RANK] = normed[rows]
        lat_in[half, :, RANK:] = turned_key[rows]

    pl.semaphore_wait(barrier, 13)

    dests = [(rr, kk) for rr in range(2) for kk in range(2)]

    def is_self(rr, kk):
        return jnp.logical_and(y == 2 * core + rr, kk == core)

    def lat_copy(rr, kk):
        return remote(
            lat_in.at[kk], lat.at[z, kk, y], y_send.at[rr, kk], y_recv.at[y],
            dev(x, kk, 2 * core + rr, z),
        )

    def q_copy(rr, kk, t):
        return remote(
            q_in.at[pair_of(kk, rr, t)], q.at[t, y], q_send.at[t, rr, kk], q_recv.at[t, y],
            dev(x, kk, 2 * core + rr, z),
        )

    def w_half(half):
        return w_in.at[:, pl.ds(512 * half, 512)]

    def w_direct(half, plus):
        to = dev(xp if plus else xm, 1 - role, y, z)
        return remote(
            w_half(half), w.at[2 * half + plus], w_send.at[half, plus], w_recv.at[2 * half + plus], to
        )

    def w_relay(half):
        t_here = 1 if half == 0 else 2
        to = dev(xp if half == 0 else xm, role, y, z)
        return remote(
            w.at[t_here], w.at[2 + half], w_send.at[half, 0], w_recv.at[2 + half], to
        )

    @pl.when(native)
    def _():
        w_direct(0, 0).start()
        w_direct(0, 1).start()
        w_direct(1, 0).start()

    for rr, kk in dests:
        @pl.when(is_self(rr, kk))
        def _():
            lat[z, kk, y] = lat_in[kk]

        @pl.when(jnp.logical_not(is_self(rr, kk)))
        def _():
            lat_copy(rr, kk).start()

    for g in range(HEADS // 2):
        plain = queries[:, g * 384:g * 384 + 128]
        left = queries[:, g * 384 + 128:g * 384 + 256].astype(F32)
        right = queries[:, g * 384 + 256:g * 384 + 384].astype(F32)
        q_in[g, 0] = plain
        q_in[g, 1] = pltpu.roll(jnp.where(lane < 64, right, left), 64, 1).astype(BF16)
        q_in[g, 2] = rotated(jnp.where(lane < 64, left, right))

    for t in range(4):
        for rr, kk in dests:
            @pl.when(is_self(rr, kk))
            def _():
                q[t, y] = q_in[pair_of(kk, rr, t)]

            @pl.when(jnp.logical_not(is_self(rr, kk)))
            def _():
                q_copy(rr, kk, t).start()

    def own_seq(yy):
        return jnp.logical_and(seq == core, yy == y)

    def source_y(i):
        return (y + AWAY[i]) % NY

    def block_of(direction, step):
        return (z + NZ - step) % NZ if direction == 0 else (z + step) % NZ

    def ring_copy(direction, step, i, have):
        piece = lat.at[block_of(direction, step - have), core, source_y(i)]
        at = (direction, step - 1, i)
        return remote(piece, piece, ring_send.at[at], ring_recv.at[at], up if direction == 0 else down)

    def ring(direction, step, i):
        return ring_copy(direction, step, i, 1)

    def pair_copy(direction, step, i, half):
        piece = lat.at[block_of(direction, step), half, source_y(i)]
        at = (direction, step, i)
        return remote(piece, piece, pair_send.at[at], pair_recv.at[at], partner)

    def carried(direction, step, i):
        return step < 4 or i // 2 == direction

    def arrive(direction, step, i):
        ring_copy(direction, step, i, 0).wait_recv()
        if step < 4 and carried(direction, step + 1, i):
            ring(direction, step + 1, i).start()
        pair_copy(direction, step, i, core).start()

    def from_partner(step):
        for direction in range(1 if step == 0 else 2):
            for i in range(4):
                if carried(direction, step, i):
                    pair_copy(direction, step, i, 1 - core).wait_recv()

    for i in range(4):
        @pl.when(jnp.logical_not(own_seq(source_y(i))))
        def _():
            remote(
                lat_in.at[0], lat.at[z, core, source_y(i)], y_send.at[0, 0], y_recv.at[source_y(i)], partner
            ).wait_recv()

        ring(0, 1, i).start()
        ring(1, 1, i).start()
        pair_copy(0, 0, i, core).start()

    def w_arrival(t):
        return remote(w.at[0], w.at[t], w_send.at[0, 0], w_recv.at[t], partner)

    m_s[...] = jnp.full_like(m_s, -jnp.inf)
    l_s[...] = jnp.zeros_like(l_s)
    acc_s[...] = jnp.zeros_like(acc_s)
    for h in range(HEADS):
        cols = slice(h * 128, (h + 1) * 128)
        v = gate[:, cols].astype(F32)
        gated[:, cols] = v / (1.0 + jnp.exp(-v))

    def unit(t, blocks):
        n = 512 * len(blocks)
        wk = jnp.concatenate([w[t, :, 0:128], w[t, :, 256:384]], axis=1)
        wv = jnp.concatenate([w[t, :, 128:256], w[t, :, 384:512]], axis=1)
        chunks = range(len(blocks))
        rows = [slice(c * 512, (c + 1) * 512) for c in chunks]

        def block(c):
            return lat[blocks[c]].reshape(512, WIDE)

        def scores(hh, c):
            turned = block(c)[:, RANK:]
            mask = lane < 64 if hh == 0 else lane >= 64
            key = jnp.concatenate(
                [k_s[rows[c], hh * 128:(hh + 1) * 128], jnp.where(mask, turned, jnp.zeros_like(turned))],
                axis=1,
            )
            s = jnp.dot(key, qt[t, hh], preferred_element_type=F32)
            s_s[hh, rows[c], :] = s
            top = s[0:8]
            for g in range(1, 64):
                top = jnp.maximum(top, s[g * 8:(g + 1) * 8])
            return top

        def peak(hh, tops):
            top = functools.reduce(jnp.maximum, tops)
            m_old = m_s[t, hh]
            m_new = jnp.maximum(m_old, jnp.max(top, axis=0, keepdims=True) * SCALE)
            m_s[t, hh] = m_new
            return m_new, jnp.exp2(m_old - m_new)

        def raise_(hh, c, m_new):
            total = jnp.zeros((8, 512), F32)
            low = jnp.broadcast_to(m_new, (8, 512))
            for g in range(32):
                row = c * 512 + g * 16
                first = jnp.exp2(s_s[hh, row:row + 8, :] * SCALE - low)
                second = jnp.exp2(s_s[hh, row + 8:row + 16, :] * SCALE - low)
                total = total + (first + second)
                p_s[hh, row:row + 16, :] = jnp.concatenate([first, second], axis=0).astype(BF16)
            return total

        def values(c):
            v = jnp.dot(block(c)[:, :RANK], wv, preferred_element_type=F32).astype(BF16)
            vt_s[:, rows[c]] = v.T

        def finish(hh, sums, shrink):
            l_s[t, hh] = l_s[t, hh] * shrink + jnp.sum(
                functools.reduce(jnp.add, sums), axis=0, keepdims=True
            )
            acc_s[t, hh] = acc_s[t, hh] * shrink + jnp.dot(
                vt_s[hh * 128:(hh + 1) * 128, :n], p_s[hh, :n], preferred_element_type=F32
            )

        for c in chunks:
            k_s[rows[c], :] = jnp.dot(block(c)[:, :RANK], wk, preferred_element_type=F32).astype(BF16)
        m_a, shrink_a = peak(0, [scores(0, c) for c in chunks])
        tops, sums_a, sums_b = [], [], []
        for c in chunks:
            tops.append(scores(1, c))
            sums_a.append(raise_(0, c, m_a))
        m_b, shrink_b = peak(1, tops)
        for c in chunks:
            values(c)
            sums_b.append(raise_(1, c, m_b))
        finish(0, sums_a, shrink_a)
        finish(1, sums_b, shrink_b)

    def o_copy(t, yy):
        return remote(
            o_buf.at[t, yy], o_ret.at[pair_of(core, role, t)], o_send.at[t, yy],
            o_recv.at[pair_of(core, role, t)], dev(x, seq, yy, z),
        )

    def o_self(yy):
        return jnp.logical_and(yy == y, seq == core)

    @pl.when(jnp.logical_not(native))
    def _():
        w_arrival(1).wait_recv()
        w_relay(0).start()

    from_partner(0)

    @pl.loop(0, len(STEP_OF))
    def _(u):
        step = pick(STEP_OF, u)
        t = pick(PLACE_OF, u)

        @pl.when(pick(FIRST_USE, u) == 1)
        def _():
            @pl.when(jnp.logical_or(native, jnp.logical_or(t == 0, t == 3)))
            def _():
                w_arrival(t).wait_recv()

            for yy in range(NY):
                @pl.when(jnp.logical_not(own_seq(yy)))
                def _():
                    remote(
                        q_in.at[0], q.at[t, yy], q_send.at[0, 0, 0], q_recv.at[t, yy], partner
                    ).wait_recv()
            for hh in range(2):
                rows = [jnp.concatenate([q[t, yy, hh], q[t, yy, 2]], axis=1) for yy in range(NY)]
                qt[t, hh] = jnp.concatenate(rows, axis=0).T

        for j, first in ((1, 2), (2, 6), (3, 12), (4, 16)):
            @pl.when(u == first)
            def _():
                from_partner(j)

        single = jnp.logical_or(step == 0, step == 4)

        @pl.when(single)
        def _():
            unit(t, [(z + step) % NZ])

        @pl.when(jnp.logical_not(single))
        def _():
            unit(t, [(z + NZ - step) % NZ, (z + step) % NZ])

        for at, what in ARRIVALS.items():
            @pl.when(u == at)
            def _():
                for j, i in what:
                    for direction in range(2):
                        if carried(direction, j, i):
                            arrive(direction, j, i)

        @pl.when(jnp.logical_and(native, u == 3))
        def _():
            w_direct(1, 1).start()

        @pl.when(jnp.logical_and(jnp.logical_not(native), u == 3))
        def _():
            w_arrival(2).wait_recv()
            w_relay(1).start()

        @pl.when(step == 4)
        def _():
            for hh in range(2):
                r = acc_s[t, hh] / l_s[t, hh]
                for yy in range(NY):
                    piece = r[:, yy * 128:(yy + 1) * 128].T.astype(BF16)
                    o_buf[t, yy, hh] = piece

                    @pl.when(o_self(yy))
                    def _():
                        o_ret[pair_of(core, role, t), hh] = piece
            for yy in range(NY):
                @pl.when(jnp.logical_not(o_self(yy)))
                def _():
                    o_copy(t, yy).start()

    total = jnp.zeros((128, 128), F32)
    for t in range(4):
        for rr, kk in dests:
            g = pair_of(kk, rr, t)

            @pl.when(jnp.logical_not(is_self(rr, kk)))
            def _():
                remote(
                    o_buf.at[0, 0], o_ret.at[g], o_send.at[0, 0], o_recv.at[g], partner
                ).wait_recv()

            for hh in range(2):
                cols = pl.ds(pl.multiple_of(g * 256 + hh * 128, 128), 128)
                piece = o_ret[g, hh].astype(F32) * gated[:, cols]
                gated[:, cols] = piece
                total = total + piece * piece
    mean = jnp.sum(total, axis=1, keepdims=True) / (HEADS * VDIM)
    scale = lax.rsqrt(mean + EPS)
    for h in range(HEADS):
        cols = slice(h * 128, (h + 1) * 128)
        out[:, cols] = (gated[:, cols] * scale * gain[:, cols]).astype(BF16)

    for rr, kk in dests:
        @pl.when(jnp.logical_not(is_self(rr, kk)))
        def _():
            lat_copy(rr, kk).wait_send()
            for t in range(4):
                q_copy(rr, kk, t).wait_send()

    @pl.when(native)
    def _():
        for half in range(2):
            for plus in range(2):
                w_direct(half, plus).wait_send()

    @pl.when(jnp.logical_not(native))
    def _():
        w_relay(0).wait_send()
        w_relay(1).wait_send()

    for i in range(4):
        pair_copy(0, 0, i, core).wait_send()
        for direction in range(2):
            for step in range(1, 5):
                if carried(direction, step, i):
                    ring(direction, step, i).wait_send()
                    pair_copy(direction, step, i, core).wait_send()
    for t in range(4):
        for yy in range(NY):
            @pl.when(jnp.logical_not(o_self(yy)))
            def _():
                o_copy(t, yy).wait_send()


def per_device(queries, latent, rope_key, latent_gain, kv_weight, gate, out_gain):
    own = queries.shape[0]
    position = lax.axis_index("sp") * own + jnp.arange(own, dtype=jnp.int32)
    half = jnp.arange(ROPE // 2, dtype=F32)
    angles = position.astype(F32)[:, None] * jnp.tile(THETA ** (-half / (ROPE // 2)), 4)[None, :]
    sign = jnp.where(jnp.arange(128) % ROPE < ROPE // 2, -1.0, 1.0)
    cosine, sine = jnp.cos(angles), jnp.sin(angles) * sign[None, :]
    any_spec = pl.BlockSpec(memory_space=pl.ANY)
    vmem_spec = pl.BlockSpec(memory_space=pltpu.VMEM)
    dma = pltpu.SemaphoreType.DMA
    return pl.pallas_call(
        body,
        out_shape=jax.ShapeDtypeStruct((own, HEADS * VDIM), BF16),
        in_specs=[vmem_spec] * 6 + [any_spec, vmem_spec, vmem_spec],
        out_specs=vmem_spec,
        scratch_shapes=[
            pltpu.VMEM((2, own // 2, WIDE), BF16),
            pltpu.VMEM((HEADS // 2, 3, 128, 128), BF16),
            pltpu.VMEM((NZ, 2, NY, 64, WIDE), BF16),
            pltpu.VMEM((4, NY, 3, 128, 128), BF16),
            pltpu.VMEM((4, 2, 256, 512), BF16),
            pltpu.VMEM((4, RANK, 512), BF16),
            pltpu.VMEM((1024, 256), BF16),
            pltpu.VMEM((256, 1024), BF16),
            pltpu.VMEM((2, 1024, 512), F32),
            pltpu.VMEM((2, 1024, 512), BF16),
            pltpu.VMEM((4, 2, 1, 512), F32),
            pltpu.VMEM((4, 2, 1, 512), F32),
            pltpu.VMEM((4, 2, 128, 512), F32),
            pltpu.VMEM((4, NY, 2, 128, 128), BF16),
            pltpu.VMEM((16, 2, 128, 128), BF16),
            pltpu.VMEM((own, HEADS * VDIM), F32),
            dma((2, 2)), dma((NY,)), dma((2, 4, 4)), dma((2, 4, 4)), dma((2, 5, 4)), dma((2, 5, 4)),
            dma((4, 2, 2)), dma((4, NY)), dma((2, 2)), dma((4,)), dma((4, NY)), dma((16,)),
        ],
        compiler_params=pltpu.CompilerParams(
            collective_id=0, has_side_effects=True, vmem_limit_bytes=60 * 2**20
        ),
        cost_estimate=pl.CostEstimate(flops=30 * 10**9, bytes_accessed=10**7, transcendentals=0),
        name="latent_attention",
    )(
        queries, latent, rope_key, latent_gain.reshape(1, -1), cosine, sine,
        kv_weight, gate, out_gain.reshape(1, -1),
    )


def solution(mesh):
    return jax.shard_map(
        per_device,
        mesh=mesh,
        in_specs=(
            P(("dp", "sp"), None),
            P(("dp", "sp"), None),
            P(("dp", "sp"), None),
            P(),
            P(None, "dp"),
            P(("dp", "sp"), None),
            P(),
        ),
        out_specs=P(("dp", "sp"), None),
        check_vma=False,
    )
```

```python
import functools

import jax
import jax.numpy as jnp
from jax import lax
from jax.experimental import pallas as pl
from jax.experimental.pallas import tpu as pltpu
from jax.sharding import PartitionSpec as P

HEADS = 32
NOPE = 128
ROPE = 64
VDIM = 128
RANK = 1024
EPS = 1e-06
THETA = 10000.0
LOG2E = 1.4426950408889634
SCALE = (NOPE + ROPE) ** (-0.5) * LOG2E
NX, NY, NZ = 4, 4, 8
WIDE = RANK + 128
NT = (((1,), (1,)), ((), ()))
BF16 = jnp.bfloat16
AWAY = (0, 1, 3, 2)
STEP_OF = (0, 0, 1, 1, 0, 1, 2, 2, 2, 0, 1, 2, 3, 3, 3, 3, 4, 4, 4, 4, 5, 5, 5, 5)
PLACE_OF = (0, 1, 0, 1, 2, 2, 0, 1, 2, 3, 3, 3, 0, 1, 2, 3, 0, 1, 2, 3, 0, 1, 2, 3)
FIRST_USE = tuple(int(t not in PLACE_OF[:u]) for u, t in enumerate(PLACE_OF))
ARRIVALS = {
    0: ((1, 0), (1, 1)), 1: ((1, 2), (1, 3)),
    2: ((2, 0),), 3: ((2, 1),), 4: ((2, 2),), 5: ((2, 3),),
    7: ((3, 0),), 8: ((3, 1),), 12: ((3, 2),), 13: ((3, 3),),
    16: ((4, 0), (4, 2)), 17: ((4, 1), (4, 3)),
}
F32 = jnp.float32


def pick(table, index):
    value = jnp.int32(table[0])
    for i, entry in enumerate(table[1:], 1):
        value = jnp.where(index == i, jnp.int32(entry), value)
    return value


def body(
    queries, latent, rope_key, latent_gain, cosine, sine, w_in, gate, gain, out,
    lat_in, q_in, lat, q, qt, w, k_s, vt_s, s_s, p_s, m_s, l_s, acc_s, o_buf, o_ret, gated,
    y_send, y_recv, ring_send, ring_recv, pair_send, pair_recv,
    q_send, q_recv, w_send, w_recv, o_send, o_recv,
):
    sp, dp = lax.axis_index("sp"), lax.axis_index("dp")
    z, y = sp // NY, sp % NY
    x, core = dp // 2, dp % 2
    seq, role = y // 2, y % 2
    native = core == role
    zp, zm = (z + 1) % NZ, (z + NZ - 1) % NZ
    xp, xm = (x + 1) % NX, (x + NX - 1) % NX

    def dev(x_, core_, y_, z_):
        return {"sp": z_ * NY + y_, "dp": x_ * 2 + core_}

    def remote(src, dst, send, recv, to):
        return pltpu.make_async_remote_copy(
            src_ref=src, dst_ref=dst, send_sem=send, recv_sem=recv,
            device_id=to, device_id_type=pl.DeviceIdType.MESH,
        )

    partner = dev(x, 1 - core, y, z)
    up, down = dev(x, core, y, zp), dev(x, core, y, zm)

    def pair_of(core_, role_, t):
        is_native = core_ == role_
        slot = jnp.where(is_native, t // 2, t % 2)
        half = jnp.where(is_native, t % 2, t // 2)
        off = jnp.where(is_native, 2 * slot, 2 * slot + 1)
        return (2 * ((x + off) % NX) + role_) * 2 + half

    barrier = pltpu.get_barrier_semaphore()
    for yy in range(NY):
        for cc in range(2):
            @pl.when(jnp.logical_or(yy != y, cc != core))
            def _():
                pl.semaphore_signal(barrier, inc=1, device_id=dev(x, cc, yy, z), device_id_type=pl.DeviceIdType.MESH)
    for to in (up, down, dev(xp, 0, y, z), dev(xp, 1, y, z), dev(xm, 0, y, z), dev(xm, 1, y, z)):
        pl.semaphore_signal(barrier, inc=1, device_id=to, device_id_type=pl.DeviceIdType.MESH)

    @pl.when(native)
    def _():
        for half in range(2):
            pltpu.make_async_copy(w_in.at[:, pl.ds(512 * half, 512)], w.at[half], w_recv.at[half]).start()

    lane = lax.broadcasted_iota(jnp.int32, (1, 128), 1)

    def rotated(pair):
        other = jnp.where(lane % 64 < 32, pltpu.roll(pair, 96, 1), pltpu.roll(pair, 32, 1))
        return (pair * cosine[...] + other * sine[...]).astype(BF16)

    wide = latent[...].astype(F32)
    level = lax.rsqrt(jnp.mean(wide * wide, axis=1, keepdims=True) + EPS)
    normed = (wide * level * latent_gain[...]).astype(BF16)
    key = rope_key[...].astype(F32)
    turned_key = rotated(jnp.concatenate([key, key], axis=1))
    for half in range(2):
        rows = slice(half * 64, (half + 1) * 64)
        lat_in[half, :, :RANK] = normed[rows]
        lat_in[half, :, RANK:] = turned_key[rows]

    pl.semaphore_wait(barrier, 13)

    dests = [(rr, kk) for rr in range(2) for kk in range(2)]

    def is_self(rr, kk):
        return jnp.logical_and(y == 2 * core + rr, kk == core)

    def lat_copy(rr, kk):
        return remote(
            lat_in.at[kk], lat.at[z, kk, y], y_send.at[rr, kk], y_recv.at[y],
            dev(x, kk, 2 * core + rr, z),
        )

    def q_copy(rr, kk, t):
        return remote(
            q_in.at[pair_of(kk, rr, t)], q.at[t, y], q_send.at[t, rr, kk], q_recv.at[t, y],
            dev(x, kk, 2 * core + rr, z),
        )

    def w_half(half):
        return w_in.at[:, pl.ds(512 * half, 512)]

    def w_direct(half, plus):
        to = dev(xp if plus else xm, 1 - role, y, z)
        return remote(
            w_half(half), w.at[2 * half + plus], w_send.at[half, plus], w_recv.at[2 * half + plus], to
        )

    def w_relay(half):
        t_here = 1 if half == 0 else 2
        to = dev(xp if half == 0 else xm, role, y, z)
        return remote(
            w.at[t_here], w.at[2 + half], w_send.at[half, 0], w_recv.at[2 + half], to
        )

    @pl.when(native)
    def _():
        w_direct(0, 0).start()
        w_direct(0, 1).start()
        w_direct(1, 0).start()

    for rr, kk in dests:
        @pl.when(is_self(rr, kk))
        def _():
            lat[z, kk, y] = lat_in[kk]

        @pl.when(jnp.logical_not(is_self(rr, kk)))
        def _():
            lat_copy(rr, kk).start()

    for g in range(HEADS // 2):
        plain = queries[:, g * 384:g * 384 + 128]
        left = queries[:, g * 384 + 128:g * 384 + 256].astype(F32)
        right = queries[:, g * 384 + 256:g * 384 + 384].astype(F32)
        q_in[g, 0] = plain
        q_in[g, 1] = pltpu.roll(jnp.where(lane < 64, right, left), 64, 1).astype(BF16)
        q_in[g, 2] = rotated(jnp.where(lane < 64, left, right))

    for t in range(4):
        for rr, kk in dests:
            @pl.when(is_self(rr, kk))
            def _():
                q[t, y] = q_in[pair_of(kk, rr, t)]

            @pl.when(jnp.logical_not(is_self(rr, kk)))
            def _():
                q_copy(rr, kk, t).start()

    def own_seq(yy):
        return jnp.logical_and(seq == core, yy == y)

    def source_y(i):
        return (y + AWAY[i]) % NY

    def block_of(direction, step):
        return (z + NZ - step) % NZ if direction == 0 else (z + step) % NZ

    def ring_copy(direction, step, i, have):
        piece = lat.at[block_of(direction, step - have), core, source_y(i)]
        at = (direction, step - 1, i)
        return remote(piece, piece, ring_send.at[at], ring_recv.at[at], up if direction == 0 else down)

    def ring(direction, step, i):
        return ring_copy(direction, step, i, 1)

    def pair_copy(direction, step, i, half):
        piece = lat.at[block_of(direction, step), half, source_y(i)]
        at = (direction, step, i)
        return remote(piece, piece, pair_send.at[at], pair_recv.at[at], partner)

    def carried(direction, step, i):
        return step < 4 or i // 2 == direction

    def arrive(direction, step, i):
        ring_copy(direction, step, i, 0).wait_recv()
        if step < 4 and carried(direction, step + 1, i):
            ring(direction, step + 1, i).start()
        pair_copy(direction, step, i, core).start()

    def from_partner(step, pieces=(0, 1, 2, 3)):
        for direction in range(1 if step == 0 else 2):
            for i in pieces:
                if carried(direction, step, i):
                    pair_copy(direction, step, i, 1 - core).wait_recv()

    for i in range(4):
        @pl.when(jnp.logical_not(own_seq(source_y(i))))
        def _():
            remote(
                lat_in.at[0], lat.at[z, core, source_y(i)], y_send.at[0, 0], y_recv.at[source_y(i)], partner
            ).wait_recv()

        ring(0, 1, i).start()
        ring(1, 1, i).start()
        pair_copy(0, 0, i, core).start()

    def w_arrival(t):
        return remote(w.at[0], w.at[t], w_send.at[0, 0], w_recv.at[t], partner)

    m_s[...] = jnp.full_like(m_s, -jnp.inf)
    l_s[...] = jnp.zeros_like(l_s)
    acc_s[...] = jnp.zeros_like(acc_s)
    for h in range(HEADS):
        cols = slice(h * 128, (h + 1) * 128)
        v = gate[:, cols].astype(F32)
        gated[:, cols] = v / (1.0 + jnp.exp(-v))

    def unit(t, blocks):
        n = 512 * len(blocks)
        wk = jnp.concatenate([w[t, :, 0:128], w[t, :, 256:384]], axis=1)
        wv = jnp.concatenate([w[t, :, 128:256], w[t, :, 384:512]], axis=1)
        chunks = range(len(blocks))
        rows = [slice(c * 512, (c + 1) * 512) for c in chunks]

        def block(c):
            return blocks[c]()

        def scores(hh, c):
            turned = block(c)[:, RANK:]
            mask = lane < 64 if hh == 0 else lane >= 64
            key = jnp.concatenate(
                [k_s[rows[c], hh * 128:(hh + 1) * 128], jnp.where(mask, turned, jnp.zeros_like(turned))],
                axis=1,
            )
            s = jnp.dot(key, qt[t, hh], preferred_element_type=F32)
            s_s[hh, rows[c], :] = s
            top = s[0:8]
            for g in range(1, 64):
                top = jnp.maximum(top, s[g * 8:(g + 1) * 8])
            return top

        def peak(hh, tops):
            top = functools.reduce(jnp.maximum, tops)
            m_old = m_s[t, hh]
            m_new = jnp.maximum(m_old, jnp.max(top, axis=0, keepdims=True) * SCALE)
            m_s[t, hh] = m_new
            return m_new, jnp.exp2(m_old - m_new)

        def raise_(hh, c, m_new):
            total = jnp.zeros((8, 512), F32)
            low = jnp.broadcast_to(m_new, (8, 512))
            for g in range(32):
                row = c * 512 + g * 16
                first = jnp.exp2(s_s[hh, row:row + 8, :] * SCALE - low)
                second = jnp.exp2(s_s[hh, row + 8:row + 16, :] * SCALE - low)
                total = total + (first + second)
                p_s[hh, row:row + 16, :] = jnp.concatenate([first, second], axis=0).astype(BF16)
            return total

        def values(c):
            v = jnp.dot(block(c)[:, :RANK], wv, preferred_element_type=F32).astype(BF16)
            vt_s[:, rows[c]] = v.T

        def finish(hh, sums, shrink):
            l_s[t, hh] = l_s[t, hh] * shrink + jnp.sum(
                functools.reduce(jnp.add, sums), axis=0, keepdims=True
            )
            acc_s[t, hh] = acc_s[t, hh] * shrink + jnp.dot(
                vt_s[hh * 128:(hh + 1) * 128, :n], p_s[hh, :n], preferred_element_type=F32
            )

        for c in chunks:
            k_s[rows[c], :] = jnp.dot(block(c)[:, :RANK], wk, preferred_element_type=F32).astype(BF16)
        m_a, shrink_a = peak(0, [scores(0, c) for c in chunks])
        tops, sums_a, sums_b = [], [], []
        for c in chunks:
            tops.append(scores(1, c))
            sums_a.append(raise_(0, c, m_a))
        m_b, shrink_b = peak(1, tops)
        for c in chunks:
            values(c)
            sums_b.append(raise_(1, c, m_b))
        finish(0, sums_a, shrink_a)
        finish(1, sums_b, shrink_b)

    def o_copy(t, yy):
        return remote(
            o_buf.at[t, yy], o_ret.at[pair_of(core, role, t)], o_send.at[t, yy],
            o_recv.at[pair_of(core, role, t)], dev(x, seq, yy, z),
        )

    def o_self(yy):
        return jnp.logical_and(yy == y, seq == core)

    @pl.when(jnp.logical_not(native))
    def _():
        w_arrival(1).wait_recv()
        w_relay(0).start()

    from_partner(0)

    @pl.loop(0, len(STEP_OF))
    def _(u):
        step = pick(STEP_OF, u)
        t = pick(PLACE_OF, u)

        @pl.when(pick(FIRST_USE, u) == 1)
        def _():
            @pl.when(jnp.logical_or(native, jnp.logical_or(t == 0, t == 3)))
            def _():
                w_arrival(t).wait_recv()

            for yy in range(NY):
                @pl.when(jnp.logical_not(own_seq(yy)))
                def _():
                    remote(
                        q_in.at[0], q.at[t, yy], q_send.at[0, 0, 0], q_recv.at[t, yy], partner
                    ).wait_recv()
            for hh in range(2):
                rows = [jnp.concatenate([q[t, yy, hh], q[t, yy, 2]], axis=1) for yy in range(NY)]
                qt[t, hh] = jnp.concatenate(rows, axis=0).T

        for j, first, pieces in (
            (1, 2, range(4)), (2, 6, range(4)), (3, 12, (0, 1)), (3, 16, (2, 3)), (4, 20, range(4))
        ):
            @pl.when(u == first)
            def _():
                from_partner(j, pieces)

        single = jnp.logical_or(step == 0, step >= 3)
        mixed = jnp.logical_or(step == 3, step == 4)

        def whole(zz):
            return lambda: lat[zz].reshape(512, WIDE)

        def parts():
            rows = []
            for k in range(4):
                alone = jnp.where(step == 5, (z + 4) % NZ, z)
                zz = jnp.where(mixed, block_of(k // 2, 3), alone)
                away = jnp.where(step == 4, AWAY[k % 2 + 2], AWAY[k % 2])
                yy = (y + jnp.where(mixed, away, AWAY[k])) % NY
                rows += [lat[zz, 0, yy], lat[zz, 1, yy]]
            return jnp.concatenate(rows, axis=0)


        @pl.when(single)
        def _():
            unit(t, [parts])

        @pl.when(jnp.logical_not(single))
        def _():
            unit(t, [whole((z + NZ - step) % NZ), whole((z + step) % NZ)])

        for at, what in ARRIVALS.items():
            @pl.when(u == at)
            def _():
                for j, i in what:
                    for direction in range(2):
                        if carried(direction, j, i):
                            arrive(direction, j, i)

        @pl.when(jnp.logical_and(native, u == 3))
        def _():
            w_direct(1, 1).start()

        @pl.when(jnp.logical_and(jnp.logical_not(native), u == 3))
        def _():
            w_arrival(2).wait_recv()
            w_relay(1).start()

        @pl.when(step == 5)
        def _():
            for hh in range(2):
                r = acc_s[t, hh] / l_s[t, hh]
                for yy in range(NY):
                    piece = r[:, yy * 128:(yy + 1) * 128].T.astype(BF16)
                    o_buf[t, yy, hh] = piece

                    @pl.when(o_self(yy))
                    def _():
                        o_ret[pair_of(core, role, t), hh] = piece
            for yy in range(NY):
                @pl.when(jnp.logical_not(o_self(yy)))
                def _():
                    o_copy(t, yy).start()

    total = jnp.zeros((128, 128), F32)
    for t in range(4):
        for rr, kk in dests:
            g = pair_of(kk, rr, t)

            @pl.when(jnp.logical_not(is_self(rr, kk)))
            def _():
                remote(
                    o_buf.at[0, 0], o_ret.at[g], o_send.at[0, 0], o_recv.at[g], partner
                ).wait_recv()

            for hh in range(2):
                cols = pl.ds(pl.multiple_of(g * 256 + hh * 128, 128), 128)
                piece = o_ret[g, hh].astype(F32) * gated[:, cols]
                gated[:, cols] = piece
                total = total + piece * piece
    mean = jnp.sum(total, axis=1, keepdims=True) / (HEADS * VDIM)
    scale = lax.rsqrt(mean + EPS)
    for h in range(HEADS):
        cols = slice(h * 128, (h + 1) * 128)
        out[:, cols] = (gated[:, cols] * scale * gain[:, cols]).astype(BF16)

    for rr, kk in dests:
        @pl.when(jnp.logical_not(is_self(rr, kk)))
        def _():
            lat_copy(rr, kk).wait_send()
            for t in range(4):
                q_copy(rr, kk, t).wait_send()

    @pl.when(native)
    def _():
        for half in range(2):
            for plus in range(2):
                w_direct(half, plus).wait_send()

    @pl.when(jnp.logical_not(native))
    def _():
        w_relay(0).wait_send()
        w_relay(1).wait_send()

    for i in range(4):
        pair_copy(0, 0, i, core).wait_send()
        for direction in range(2):
            for step in range(1, 5):
                if carried(direction, step, i):
                    ring(direction, step, i).wait_send()
                    pair_copy(direction, step, i, core).wait_send()
    for t in range(4):
        for yy in range(NY):
            @pl.when(jnp.logical_not(o_self(yy)))
            def _():
                o_copy(t, yy).wait_send()


def per_device(queries, latent, rope_key, latent_gain, kv_weight, gate, out_gain):
    own = queries.shape[0]
    position = lax.axis_index("sp") * own + jnp.arange(own, dtype=jnp.int32)
    half = jnp.arange(ROPE // 2, dtype=F32)
    angles = position.astype(F32)[:, None] * jnp.tile(THETA ** (-half / (ROPE // 2)), 4)[None, :]
    sign = jnp.where(jnp.arange(128) % ROPE < ROPE // 2, -1.0, 1.0)
    cosine, sine = jnp.cos(angles), jnp.sin(angles) * sign[None, :]
    any_spec = pl.BlockSpec(memory_space=pl.ANY)
    vmem_spec = pl.BlockSpec(memory_space=pltpu.VMEM)
    dma = pltpu.SemaphoreType.DMA
    return pl.pallas_call(
        body,
        out_shape=jax.ShapeDtypeStruct((own, HEADS * VDIM), BF16),
        in_specs=[vmem_spec] * 6 + [any_spec, vmem_spec, vmem_spec],
        out_specs=vmem_spec,
        scratch_shapes=[
            pltpu.VMEM((2, own // 2, WIDE), BF16),
            pltpu.VMEM((HEADS // 2, 3, 128, 128), BF16),
            pltpu.VMEM((NZ, 2, NY, 64, WIDE), BF16),
            pltpu.VMEM((4, NY, 3, 128, 128), BF16),
            pltpu.VMEM((4, 2, 256, 512), BF16),
            pltpu.VMEM((4, RANK, 512), BF16),
            pltpu.VMEM((1024, 256), BF16),
            pltpu.VMEM((256, 1024), BF16),
            pltpu.VMEM((2, 1024, 512), F32),
            pltpu.VMEM((2, 1024, 512), BF16),
            pltpu.VMEM((4, 2, 1, 512), F32),
            pltpu.VMEM((4, 2, 1, 512), F32),
            pltpu.VMEM((4, 2, 128, 512), F32),
            pltpu.VMEM((4, NY, 2, 128, 128), BF16),
            pltpu.VMEM((16, 2, 128, 128), BF16),
            pltpu.VMEM((own, HEADS * VDIM), F32),
            dma((2, 2)), dma((NY,)), dma((2, 4, 4)), dma((2, 4, 4)), dma((2, 5, 4)), dma((2, 5, 4)),
            dma((4, 2, 2)), dma((4, NY)), dma((2, 2)), dma((4,)), dma((4, NY)), dma((16,)),
        ],
        compiler_params=pltpu.CompilerParams(
            collective_id=0, has_side_effects=True, vmem_limit_bytes=60 * 2**20
        ),
        cost_estimate=pl.CostEstimate(flops=30 * 10**9, bytes_accessed=10**7, transcendentals=0),
        name="latent_attention",
    )(
        queries, latent, rope_key, latent_gain.reshape(1, -1), cosine, sine,
        kv_weight, gate, out_gain.reshape(1, -1),
    )


def solution(mesh):
    return jax.shard_map(
        per_device,
        mesh=mesh,
        in_specs=(
            P(("dp", "sp"), None),
            P(("dp", "sp"), None),
            P(("dp", "sp"), None),
            P(),
            P(None, "dp"),
            P(("dp", "sp"), None),
            P(),
        ),
        out_specs=P(("dp", "sp"), None),
        check_vma=False,
    )
```
